32 devices in a mesh: ra: 4 (over z), cb: 4 (over y, x), dp: 2 (over core).
Axes of the slice: x: 2, y: 2, z: 4, core: 2. Of those that a mesh axis runs over, the one named last changes fastest.
Arguments:
- tokens: bfloat16 [384, 4096], P('dp', 'ra'), may hold values from -13 to 13, as said below
- gate_first: bfloat16 [4096, 11264], P('ra', 'cb'), may hold values from -0.125 to 0.125
- up_first: bfloat16 [4096, 11264], P('ra', 'cb'), may hold values from -0.125 to 0.125
- down_first: bfloat16 [11264, 4096], P('cb', 'ra'), may hold values from -0.0546875 to 0.0546875
- gain_first: float32 [4096], P('ra'), may hold values from 0.1 to 1.9
- shift_first: float32 [4096], P('ra'), may hold values from -3 to 3
- gate_second: bfloat16 [4096, 11264], P('ra', 'cb'), may hold values from -0.125 to 0.125
- up_second: bfloat16 [4096, 11264], P('ra', 'cb'), may hold values from -0.125 to 0.125
- down_second: bfloat16 [11264, 4096], P('cb', 'ra'), may hold values from -0.0546875 to 0.0546875
- gain_second: float32 [4096], P('ra'), may hold values from 0.1 to 1.9
- shift_second: float32 [4096], P('ra'), may hold values from -3 to 3
Outputs:
- result: bfloat16 [384, 4096], P('dp', 'ra')
The draws below stay inside these ranges and needn't reach their ends.
Inputs may be any that keep to these rules, and one draw needn't show every extreme that they name: `tokens`: input activations whose blocks of 64 consecutive features have their own scale and offset.
All inputs are finite; a program needn't handle non-finite values.
Results may differ from the reference program's by a relative error of at most 0.0066.
Values may be sent and summed in bfloat16 or wider, within the bound.
A program may use at most 128 MiB of HBM per device.

```python
import jax
import jax.numpy as jnp
from jax import lax

D = 4096
FF = 11264
TOKENS = 384


def draw_tokens(key, part):
    first, second, third, fourth = jax.random.split(key, 4)
    groups = D // 64
    scales = jnp.exp(jax.random.uniform(first, (groups,), jnp.float32, jnp.log(0.25), jnp.log(3.0)))
    offsets = jax.random.uniform(second, (groups,), jnp.float32, -1.0, 1.0)
    noise = jnp.clip(jax.random.normal(third, (TOKENS, D), jnp.float32), -4.0, 4.0)
    values = noise * jnp.repeat(scales, 64)[None, :] + jnp.repeat(offsets, 64)[None, :]
    return values.astype(jnp.bfloat16)


def strengthened(drawn, own_key, source, target, parts, factor):
    def block_of(dim):
        return (jnp.arange(drawn.shape[dim]) // (drawn.shape[dim] // parts)).reshape((-1,) + (1,) * (drawn.ndim - 1 - dim))

    near = jax.random.permutation(own_key, parts)[block_of(target)]
    far = (block_of(target) + parts // 2) % parts
    return jnp.where((block_of(source) == near) | (block_of(source) == far), factor * drawn, drawn)


def level_of(key, extent, pieces, smallest, largest):
    def one(dim, blocks):
        steps = jax.random.uniform(jax.random.fold_in(jax.random.fold_in(key, 6), dim), (blocks,), jnp.float32, smallest / len(pieces), largest / len(pieces))
        return jnp.repeat(jnp.exp(steps), extent[dim] // blocks).reshape((-1,) + (1,) * (len(extent) - dim - 1))

    factor_of = one(*pieces[0])
    for cut in pieces[1:]:
        factor_of = factor_of * one(*cut)
    return factor_of


def scatter_about(stream_key, extent, spread, bound, cuts=(), dtype=jnp.bfloat16):
    level = level_of(stream_key, extent, cuts, -0.22, 0.18) if cuts else 1.0
    array = jax.random.normal(stream_key, extent, jnp.float32) * spread * level
    return jnp.minimum(jnp.maximum(array, -bound), bound).astype(dtype)


def bell_draw_with(rng, shape, scale, limit, cuts, heavy, held_as=jnp.bfloat16):
    result = scale * jax.random.normal(rng, shape, jnp.float32)
    if cuts:
        result = result * level_of(rng, shape, cuts, -0.22, 0.18)
    return jnp.clip(strengthened(result, jax.random.fold_in(rng, 3), *heavy), -limit, limit).astype(held_as)


def setup_inputs(seed: int = 0) -> dict:
    key_list = jax.random.split(jax.random.key(seed), 12)
    return {
        "tokens": draw_tokens(jax.random.fold_in(key_list[11], 71), 0),
        "gate_first": bell_draw_with(key_list[1], (D, FF), D ** -0.5, 0.125, ((0, 4), (1, 4)), (0, 1, 4, 2.0)),
        "up_first": bell_draw_with(key_list[2], (D, FF), D ** -0.5, 0.125, ((0, 4), (1, 4)), (0, 1, 4, 2.0)),
        "down_first": scatter_about(key_list[3], (FF, D), FF ** -0.5, 0.0546875, ((0, 4), (1, 4))),
        "gain_first": jnp.clip(1.0 + 0.18 * jax.random.normal(key_list[4], (D,), jnp.float32), 0.1, 1.9),
        "shift_first": scatter_about(key_list[5], (D,), 0.5, 3.0, ((0, 4),), jnp.float32),
        "gate_second": bell_draw_with(key_list[6], (D, FF), D ** -0.5, 0.125, ((0, 4), (1, 4)), (0, 1, 4, 2.0)),
        "up_second": bell_draw_with(key_list[7], (D, FF), D ** -0.5, 0.125, ((0, 4), (1, 4)), (0, 1, 4, 2.0)),
        "down_second": scatter_about(key_list[8], (FF, D), FF ** -0.5, 0.0546875, ((0, 4), (1, 4))),
        "gain_second": jnp.clip(1.0 + 0.18 * jax.random.normal(key_list[9], (D,), jnp.float32), 0.1, 1.9),
        "shift_second": scatter_about(key_list[10], (D,), 0.5, 3.0, ((0, 4),), jnp.float32),
    }


def normalize(mixed, gain, bias):
    mean = lax.optimization_barrier(jnp.mean(mixed, axis=-1, keepdims=True))
    variance = lax.optimization_barrier(jnp.mean(jnp.square(mixed - mean), axis=-1, keepdims=True))
    return (mixed - mean) * jax.lax.rsqrt(variance + 1e-05) * gain + bias

def half_step(values, gate, up, down, gain, bias):
    gate_pre = jnp.dot(values, gate, preferred_element_type=jnp.float32)
    up_pre = jnp.dot(values, up, preferred_element_type=jnp.float32)
    hidden = (jax.nn.silu(gate_pre) * up_pre).astype(jnp.bfloat16)
    branch = jnp.dot(hidden, down, preferred_element_type=jnp.float32)
    mixed = 0.25 * values.astype(jnp.float32) + 0.5 * branch
    return normalize(mixed, gain, bias).astype(jnp.bfloat16)

def reference(tokens, gate_first, up_first, down_first, gain_first, shift_first, gate_second, up_second, down_second, gain_second, shift_second):
    middle = half_step(tokens, gate_first, up_first, down_first, gain_first, shift_first)
    return half_step(middle, gate_second, up_second, down_second, gain_second, shift_second)
```

```python
import functools

import jax
import jax.numpy as jnp
from jax import lax
from jax.experimental import pallas as pl
from jax.experimental.pallas import tpu as pltpu
from jax.sharding import PartitionSpec as P

F32 = jnp.float32
BF16 = jnp.bfloat16
SKEW = 2
FLOW = (F32, BF16)
FOLD = (F32, F32)
LAYERS = 2


def dot(a, b):
    return jnp.dot(a, b, preferred_element_type=F32)


def kernel(
    R, C, D, chunks, width,
    tokens, g0, u0, d0, gain0, shift0, g1, u1, d1, gain1, shift1,
    out,
    v, wg, wu, wd, part, flow0, flow1, hid, acc, cs0, cs1, cr0, cr1, stat,
    sem_v, sem_g, sem_u, sem_d,
    flow_s, flow_r, hid_s, hid_r, fold_s, fold_r, stat_s, stat_r,
):
    r = lax.axis_index("ra")
    c = lax.axis_index("cb")
    rows = tokens.shape[0]
    half = rows // 2
    bits = C.bit_length() - 1
    gates, ups, downs = (g0, g1), (u0, u1), (d0, d1)
    gains, shifts = (gain0, gain1), (shift0, shift1)
    flows, css, crs = (flow0, flow1), (cs0, cs1), (cr0, cr1)

    def partner(k):
        m = 2**k
        return c + m - 2 * m * ((c // m) % 2)

    load_v = pltpu.make_async_copy(tokens, v, sem_v)
    load_v.start()

    def load_gate(l, j):
        return pltpu.make_async_copy(
            gates[l].at[:, pl.ds(pl.multiple_of(j * width, width), width)], wg.at[l, j], sem_g.at[l, j]
        )

    def load_up(l, j):
        return pltpu.make_async_copy(
            ups[l].at[:, pl.ds(pl.multiple_of(j * width, width), width)], wu.at[l, j], sem_u.at[l, j]
        )

    def load_down(l, j):
        return pltpu.make_async_copy(
            downs[l].at[pl.ds(pl.multiple_of(j * width, width), width)], wd.at[l, j], sem_d.at[l, j]
        )

    def begin(l):
        @pl.loop(0, chunks)
        def _(j):
            load_gate(l, j).start()
            load_up(l, j).start()

        @pl.loop(0, chunks)
        def _(j):
            load_down(l, j).start()

    begin(0)

    barrier = pltpu.get_barrier_semaphore()
    for o in range(1, R):
        pl.semaphore_signal(barrier, inc=1, device_id={"ra": (r + o) % R})
    for k in range(bits):
        pl.semaphore_signal(barrier, inc=1, device_id={"cb": partner(k)})
    pl.semaphore_wait(barrier, R - 1 + bits)

    load_v.wait()

    for l in range(LAYERS):
        flow, cs, cr = flows[l], css[l], crs[l]

        def step_of(d):
            return 1 - 2 * d

        def send_flow(d, j):
            return pltpu.make_async_remote_copy(
                src_ref=flow.at[d, j], dst_ref=flow.at[d, j],
                send_sem=flow_s.at[l, d, j], recv_sem=flow_r.at[l, d, j],
                device_id={"ra": (r + step_of(d) + R) % R},
            )

        def send_hid(d, j):
            return pltpu.make_async_remote_copy(
                src_ref=hid.at[l, d, j], dst_ref=hid.at[l, d, j],
                send_sem=hid_s.at[l, d, j], recv_sem=hid_r.at[l, d, j],
                device_id={"ra": (r - step_of(d) + R) % R},
            )

        @pl.loop(0, chunks)
        def _(j):
            load_gate(l, j).wait()
            load_up(l, j).wait()
            gate_part = dot(v[...], wg[l, j])
            up_part = dot(v[...], wu[l, j])
            for d in range(2):
                lo = (1 - d) * half
                first = r == d * (R - 1)
                a = gate_part[lo:lo + half]
                b = up_part[lo:lo + half]

                @pl.when(first)
                def _():
                    flow[d, j, :, :width] = a.astype(flow.dtype)
                    flow[d, j, :, width:] = b.astype(flow.dtype)
                    send_flow(d, j).start()

                @pl.when(jnp.logical_not(first))
                def _():
                    part[d, j, :, :width] = a
                    part[d, j, :, width:] = b

        if l + 1 < LAYERS:
            begin(l + 1)

        acc[...] = jnp.zeros_like(acc)

        @pl.loop(0, chunks)
        def _(j):
            load_down(l, j).wait()

        @pl.loop(0, chunks + 2 * (R - 1) * SKEW)
        def _(t):
            for d in range(2):
                place = r if d == 0 else R - 1 - r
                j = t - place * SKEW

                @pl.when((place > 0) & (j >= 0) & (j < chunks))
                def _():
                    send_flow(d, j).wait_recv()
                    total = flow[d, j].astype(F32) + part[d, j]

                    @pl.when(place < R - 1)
                    def _():
                        flow[d, j] = total.astype(flow.dtype)
                        send_flow(d, j).start()

                    @pl.when(place == R - 1)
                    def _():
                        gate_pre = total[:, :width]
                        up_pre = total[:, width:]
                        hid[l, d, j] = (jax.nn.silu(gate_pre) * up_pre).astype(BF16)

            for d in range(2):
                place = r if d == 0 else R - 1 - r
                back = R - 1 - place
                i = t - (R - 1) * SKEW - back * SKEW

                @pl.when((i >= 0) & (i < chunks))
                def _():
                    @pl.when(back > 0)
                    def _():
                        send_hid(d, i).wait_recv()

                    @pl.when(place > 0)
                    def _():
                        send_hid(d, i).start()

                    acc[d] += dot(hid[l, d, i], wd[l, i])

        def send_fold(d, k):
            return pltpu.make_async_remote_copy(
                src_ref=cs.at[d, k], dst_ref=cr.at[d, k],
                send_sem=fold_s.at[l, d, k], recv_sem=fold_r.at[l, d, k],
                device_id={"cb": partner((k + d) % bits)},
            )

        for d in range(2):
            cs[d, 0] = acc[d].astype(cs.dtype)
            send_fold(d, 0).start()
        for k in range(bits):
            for d in range(2):
                send_fold(d, k).wait_recv()
                total = cs[d, k].astype(F32) + cr[d, k].astype(F32)
                if k + 1 < bits:
                    cs[d, k + 1] = total.astype(cs.dtype)
                    send_fold(d, k + 1).start()
                else:
                    lo = (1 - d) * half
                    acc[d] = 0.25 * v[lo:lo + half].astype(F32) + 0.5 * total

        padded = stat.shape[-1]
        sums = []
        for d in (1, 0):
            m = acc[d]
            sums.append((jnp.sum(m, axis=-1, keepdims=True), jnp.sum(m * m, axis=-1, keepdims=True)))
        ones = jnp.concatenate([s[0] for s in sums] + ([jnp.zeros((padded - rows, 1), F32)] if padded > rows else []))
        twos = jnp.concatenate([s[1] for s in sums] + ([jnp.zeros((padded - rows, 1), F32)] if padded > rows else []))
        lane = lax.broadcasted_iota(jnp.int32, (padded, 128), 1)
        mine = jnp.where(lane == 0, ones, twos).T[:8]
        stat[l, r] = mine

        def send_stat(o):
            return pltpu.make_async_remote_copy(
                src_ref=stat.at[l, r], dst_ref=stat.at[l, r],
                send_sem=stat_s.at[l, o], recv_sem=stat_r.at[l, r],
                device_id={"ra": (r + o) % R},
            )

        def recv_stat(o):
            src = (r + o) % R
            return pltpu.make_async_remote_copy(
                src_ref=stat.at[l, src], dst_ref=stat.at[l, src],
                send_sem=stat_s.at[l, o], recv_sem=stat_r.at[l, src],
                device_id={"ra": src},
            )

        for o in range(1, R):
            send_stat(o).start()
        @pl.loop(0, chunks)
        def _(j):
            for d in range(2):
                place = r if d == 0 else R - 1 - r

                @pl.when(place < R - 1)
                def _():
                    send_flow(d, j).wait_send()

                @pl.when(place > 0)
                def _():
                    send_hid(d, j).wait_send()

        for d in range(2):
            for k in range(bits):
                send_fold(d, k).wait_send()
        for o in range(1, R):
            recv_stat(o).wait_recv()
        whole = stat[l, 0]
        for q in range(1, R):
            whole = whole + stat[l, q]
        mean = whole / D
        row = lax.broadcasted_iota(jnp.int32, whole.shape, 0)
        variance = mean - jnp.where(row == 1, 1.0, 0.0) * (mean[:1] * mean[:1])
        both = jnp.where(row == 1, lax.rsqrt(variance + 1e-05), mean)
        cols = jnp.concatenate([both] * 16, axis=0).T
        target = v if l + 1 < LAYERS else out
        for d in range(2):
            lo = (1 - d) * half
            centre = cols[lo:lo + half, 0:1]
            scale = cols[lo:lo + half, 1:2]
            normed = (acc[d] - centre) * scale * gains[l][...] + shifts[l][...]
            target[lo:lo + half] = normed.astype(BF16)
        for o in range(1, R):
            send_stat(o).wait_send()


def on_device(R, C, D, *args):
    tokens, g0, u0, d0, a0, b0, g1, u1, d1, a1, b1 = args
    rows, depth = tokens.shape
    ff = g0.shape[1]
    width = 256 if ff % 256 == 0 else 128
    chunks = ff // width
    half = rows // 2
    bits = C.bit_length() - 1
    padded = -(-rows // 128) * 128
    vmem = pl.BlockSpec(memory_space=pltpu.VMEM)
    hbm = pl.BlockSpec(memory_space=pl.ANY)
    L = LAYERS
    dma = pltpu.SemaphoreType.DMA
    line = lambda x: x.reshape(1, depth)
    return pl.pallas_call(
        functools.partial(kernel, R, C, D, chunks, width),
        out_shape=jax.ShapeDtypeStruct((rows, depth), BF16),
        in_specs=[hbm, hbm, hbm, hbm, vmem, vmem, hbm, hbm, hbm, vmem, vmem],
        out_specs=vmem,
        scratch_shapes=[
            pltpu.VMEM((rows, depth), BF16),
            pltpu.VMEM((L, chunks, depth, width), BF16),
            pltpu.VMEM((L, chunks, depth, width), BF16),
            pltpu.VMEM((L, chunks, width, depth), BF16),
            pltpu.VMEM((2, chunks, half, 2 * width), F32),
            pltpu.VMEM((2, chunks, half, 2 * width), FLOW[0]),
            pltpu.VMEM((2, chunks, half, 2 * width), FLOW[1]),
            pltpu.VMEM((L, 2, chunks, half, width), BF16),
            pltpu.VMEM((2, half, depth), F32),
            pltpu.VMEM((2, bits, half, depth), FOLD[0]),
            pltpu.VMEM((2, bits, half, depth), FOLD[1]),
            pltpu.VMEM((2, bits, half, depth), FOLD[0]),
            pltpu.VMEM((2, bits, half, depth), FOLD[1]),
            pltpu.VMEM((L, R, 8, padded), F32),
            dma,
            dma((L, chunks)),
            dma((L, chunks)),
            dma((L, chunks)),
            dma((L, 2, chunks)),
            dma((L, 2, chunks)),
            dma((L, 2, chunks)),
            dma((L, 2, chunks)),
            dma((L, 2, bits)),
            dma((L, 2, bits)),
            dma((L, R)),
            dma((L, R)),
        ],
        compiler_params=pltpu.CompilerParams(
            collective_id=0, has_side_effects=True, vmem_limit_bytes=67043328
        ),
    )(tokens, g0, u0, d0, line(a0), line(b0), g1, u1, d1, line(a1), line(b1))


def solution(mesh):
    in_specs = (
        P("dp", "ra"),
        P("ra", "cb"),
        P("ra", "cb"),
        P("cb", "ra"),
        P("ra"),
        P("ra"),
        P("ra", "cb"),
        P("ra", "cb"),
        P("cb", "ra"),
        P("ra"),
        P("ra"),
    )

    def step(tokens, *rest):
        R, C = mesh.shape["ra"], mesh.shape["cb"]
        return on_device(R, C, tokens.shape[1] * R, tokens, *rest)

    return jax.shard_map(
        step, mesh=mesh, in_specs=in_specs, out_specs=P("dp", "ra"), check_vma=False
    )
```

```python
import functools

import jax
import jax.numpy as jnp
from jax import lax
from jax.experimental import pallas as pl
from jax.experimental.pallas import tpu as pltpu
from jax.sharding import PartitionSpec as P

F32 = jnp.float32
BF16 = jnp.bfloat16
SKEW = 3
NARROW = (4, 11)
FOLD = (F32, BF16)
LAYERS = 2
GROUPS = 1


def dot(a, b):
    return jnp.dot(a, b, preferred_element_type=F32)


def kernel(
    R, C, D, chunks, width,
    tokens, g0, u0, d0, gain0, shift0, g1, u1, d1, gain1, shift1,
    out,
    v, wg, wu, wd, part, flow0, flow0n, flow1, hid, acc, cs0, cs1, cr0, cr1, stat,
    sem_v, sem_g, sem_u, sem_d,
    flow_s, flow_r, hid_s, hid_r, fold_s, fold_r, stat_s, stat_r,
):
    r = lax.axis_index("ra")
    c = lax.axis_index("cb")
    rows = tokens.shape[0]
    span = rows // GROUPS
    half = span // 2
    total_chunks = GROUPS * chunks
    bits = C.bit_length() - 1
    gates, ups, downs = (g0, g1), (u0, u1), (d0, d1)
    gains, shifts = (gain0, gain1), (shift0, shift1)
    css, crs = (cs0, cs1), (cr0, cr1)
    narrow = flow0n.shape[1]
    flows = (
        ((flow0n, 0, narrow), (flow0, narrow, total_chunks)),
        ((flow1, 0, total_chunks),),
    )

    def partner(k):
        m = 2**k
        return c + m - 2 * m * ((c // m) % 2)

    load_v = pltpu.make_async_copy(tokens, v, sem_v)
    load_v.start()

    def load_gate(l, j):
        return pltpu.make_async_copy(
            gates[l].at[:, pl.ds(pl.multiple_of(j * width, width), width)], wg.at[l, j], sem_g.at[l, j]
        )

    def load_up(l, j):
        return pltpu.make_async_copy(
            ups[l].at[:, pl.ds(pl.multiple_of(j * width, width), width)], wu.at[l, j], sem_u.at[l, j]
        )

    def load_down(l, j):
        return pltpu.make_async_copy(
            downs[l].at[pl.ds(pl.multiple_of(j * width, width), width)], wd.at[l, j], sem_d.at[l, j]
        )

    def begin(l):
        @pl.loop(0, chunks)
        def _(j):
            load_gate(l, j).start()
            load_up(l, j).start()

        @pl.loop(0, chunks)
        def _(j):
            load_down(l, j).start()

    begin(0)

    barrier = pltpu.get_barrier_semaphore()
    for o in range(1, R):
        pl.semaphore_signal(barrier, inc=1, device_id={"ra": (r + o) % R})
    for k in range(bits):
        pl.semaphore_signal(barrier, inc=1, device_id={"cb": partner(k)})
    pl.semaphore_wait(barrier, R - 1 + bits)

    load_v.wait()

    def step_of(d):
        return 1 - 2 * d

    def send_flow(l, d, q, ref, lo):
        return pltpu.make_async_remote_copy(
            src_ref=ref.at[d, q - lo], dst_ref=ref.at[d, q - lo],
            send_sem=flow_s.at[l, d, q], recv_sem=flow_r.at[l, d, q],
            device_id={"ra": (r + step_of(d) + R) % R},
        )

    def send_hid(l, d, q):
        return pltpu.make_async_remote_copy(
            src_ref=hid.at[l, d, q], dst_ref=hid.at[l, d, q],
            send_sem=hid_s.at[l, d, q], recv_sem=hid_r.at[l, d, q],
            device_id={"ra": (r - step_of(d) + R) % R},
        )

    def expand(l, first_group, groups, fresh):
        top = first_group * span

        @pl.loop(0, chunks)
        def _(j):
            if fresh:
                load_gate(l, j).wait()
                load_up(l, j).wait()
            x = v[top:top + groups * span]
            gate_part = dot(x, wg[l, j])
            up_part = dot(x, wu[l, j])
            for g in range(groups):
                q = (first_group + g) * chunks + j
                for d in range(2):
                    lo = g * span + (1 - d) * half
                    first = r == d * (R - 1)
                    a = gate_part[lo:lo + half]
                    b = up_part[lo:lo + half]

                    for flow, begins, ends in flows[l]:
                        @pl.when(first & (q >= begins) & (q < ends))
                        def _():
                            flow[d, q - begins, :, :width] = a.astype(flow.dtype)
                            flow[d, q - begins, :, width:] = b.astype(flow.dtype)
                            send_flow(l, d, q, flow, begins).start()

                    @pl.when(jnp.logical_not(first))
                    def _():
                        part[d, q, :, :width] = a
                        part[d, q, :, width:] = b

    def send_fold(l, g, d, k):
        return pltpu.make_async_remote_copy(
            src_ref=css[l].at[g, d, k], dst_ref=crs[l].at[g, d, k],
            send_sem=fold_s.at[l, g, d, k], recv_sem=fold_r.at[l, g, d, k],
            device_id={"cb": partner((k + d) % bits)},
        )

    def fold_begin(l, g):
        for d in range(2):
            css[l][g, d, 0] = acc[g, d].astype(css[l].dtype)
            send_fold(l, g, d, 0).start()

    def fold_step(l, g, k):
        cs, cr = css[l], crs[l]
        for d in range(2):
            send_fold(l, g, d, k).wait_recv()
            total = cs[g, d, k].astype(F32) + cr[g, d, k].astype(F32)
            if k + 1 < bits:
                cs[g, d, k + 1] = total.astype(cs.dtype)
                send_fold(l, g, d, k + 1).start()
            else:
                lo = g * span + (1 - d) * half
                acc[g, d] = 0.25 * v[lo:lo + half].astype(F32) + 0.5 * total
        if k + 1 == bits:
            stat_begin(l, g)

    def send_stat(l, g, o):
        return pltpu.make_async_remote_copy(
            src_ref=stat.at[l, g, r], dst_ref=stat.at[l, g, r],
            send_sem=stat_s.at[l, g, o], recv_sem=stat_r.at[l, g, r],
            device_id={"ra": (r + o) % R},
        )

    def recv_stat(l, g, o):
        src = (r + o) % R
        return pltpu.make_async_remote_copy(
            src_ref=stat.at[l, g, src], dst_ref=stat.at[l, g, src],
            send_sem=stat_s.at[l, g, o], recv_sem=stat_r.at[l, g, src],
            device_id={"ra": src},
        )

    def stat_begin(l, g):
        padded = stat.shape[-1]
        sums = []
        for d in (1, 0):
            m = acc[g, d]
            sums.append((jnp.sum(m, axis=-1, keepdims=True), jnp.sum(m * m, axis=-1, keepdims=True)))
        rest = [jnp.zeros((padded - span, 1), F32)] if padded > span else []
        ones = jnp.concatenate([s[0] for s in sums] + rest)
        twos = jnp.concatenate([s[1] for s in sums] + rest)
        lane = lax.broadcasted_iota(jnp.int32, (padded, 128), 1)
        stat[l, g, r] = jnp.where(lane == 0, ones, twos).T[:8]
        for o in range(1, R):
            send_stat(l, g, o).start()

    def finish(l, g):
        for o in range(1, R):
            recv_stat(l, g, o).wait_recv()
        whole = stat[l, g, 0]
        for q in range(1, R):
            whole = whole + stat[l, g, q]
        mean = whole / D
        row = lax.broadcasted_iota(jnp.int32, whole.shape, 0)
        variance = mean - jnp.where(row == 1, 1.0, 0.0) * (mean[:1] * mean[:1])
        both = jnp.where(row == 1, lax.rsqrt(variance + 1e-05), mean)
        cols = jnp.concatenate([both] * 16, axis=0).T
        target = v if l + 1 < LAYERS else out
        for d in range(2):
            lo = (1 - d) * half
            centre = cols[lo:lo + half, 0:1]
            scale = cols[lo:lo + half, 1:2]
            normed = (acc[g, d] - centre) * scale * gains[l][...] + shifts[l][...]
            target[g * span + lo:g * span + lo + half] = normed.astype(BF16)

    expand(0, 0, GROUPS, True)
    last = GROUPS - 1
    lag = chunks + 2 * (R - 1) * SKEW
    gap = max(1, chunks // (bits + 1))
    steps = max(total_chunks + 2 * (R - 1) * SKEW, lag + last * chunks - chunks + gap * (bits + 1) + 1)
    for l in range(LAYERS):
        if l + 1 < LAYERS:
            begin(l + 1)

        acc[...] = jnp.zeros_like(acc)

        @pl.loop(0, chunks)
        def _(j):
            load_down(l, j).wait()

        @pl.loop(0, steps)
        def _(t):
            for d in range(2):
                place = r if d == 0 else R - 1 - r
                j = t - place * SKEW

                for flow, begins, ends in flows[l]:
                    @pl.when((place > 0) & (j >= begins) & (j < ends))
                    def _():
                        send_flow(l, d, j, flow, begins).wait_recv()
                        total = flow[d, j - begins].astype(F32) + part[d, j]

                        @pl.when(place < R - 1)
                        def _():
                            flow[d, j - begins] = total.astype(flow.dtype)
                            send_flow(l, d, j, flow, begins).start()

                        @pl.when(place == R - 1)
                        def _():
                            gate_pre = total[:, :width]
                            up_pre = total[:, width:]
                            hid[l, d, j] = (jax.nn.silu(gate_pre) * up_pre).astype(BF16)

            for d in range(2):
                place = r if d == 0 else R - 1 - r
                back = R - 1 - place
                i = t - (R - 1) * SKEW - back * SKEW

                @pl.when((i >= 0) & (i < total_chunks))
                def _():
                    @pl.when(back > 0)
                    def _():
                        send_hid(l, d, i).wait_recv()

                    @pl.when(place > 0)
                    def _():
                        send_hid(l, d, i).start()

                    g = i // chunks
                    acc[g, d] += dot(hid[l, d, i], wd[l, i - g * chunks])

            for g in range(last):
                at = lag + g * chunks

                @pl.when(t == at)
                def _():
                    fold_begin(l, g)

                for k in range(bits):
                    @pl.when(t == at + gap * (k + 1))
                    def _():
                        fold_step(l, g, k)

                @pl.when(t == at + gap * (bits + 1))
                def _():
                    finish(l, g)

        fold_begin(l, last)
        if l + 1 < LAYERS and last > 0:
            expand(l + 1, 0, last, True)
        for k in range(bits):
            fold_step(l, last, k)

        @pl.loop(0, total_chunks)
        def _(j):
            for d in range(2):
                place = r if d == 0 else R - 1 - r

                for flow, begins, ends in flows[l]:
                    @pl.when((place < R - 1) & (j >= begins) & (j < ends))
                    def _():
                        send_flow(l, d, j, flow, begins).wait_send()

                @pl.when(place > 0)
                def _():
                    send_hid(l, d, j).wait_send()

        finish(l, last)
        if l + 1 < LAYERS:
            expand(l + 1, last, 1, last == 0)
        for g in range(GROUPS):
            for d in range(2):
                for k in range(bits):
                    send_fold(l, g, d, k).wait_send()
            for o in range(1, R):
                send_stat(l, g, o).wait_send()


def on_device(R, C, D, *args):
    tokens, g0, u0, d0, a0, b0, g1, u1, d1, a1, b1 = args
    rows, depth = tokens.shape
    ff = g0.shape[1]
    width = 256 if ff % 256 == 0 else 128
    chunks = ff // width
    span = rows // GROUPS
    half = span // 2
    bits = C.bit_length() - 1
    padded = -(-span // 128) * 128
    Q = GROUPS * chunks
    narrow = Q * NARROW[0] // NARROW[1]
    vmem = pl.BlockSpec(memory_space=pltpu.VMEM)
    hbm = pl.BlockSpec(memory_space=pl.ANY)
    L = LAYERS
    dma = pltpu.SemaphoreType.DMA
    line = lambda x: x.reshape(1, depth)
    return pl.pallas_call(
        functools.partial(kernel, R, C, D, chunks, width),
        out_shape=jax.ShapeDtypeStruct((rows, depth), BF16),
        in_specs=[hbm, hbm, hbm, hbm, vmem, vmem, hbm, hbm, hbm, vmem, vmem],
        out_specs=vmem,
        scratch_shapes=[
            pltpu.VMEM((rows, depth), BF16),
            pltpu.VMEM((L, chunks, depth, width), BF16),
            pltpu.VMEM((L, chunks, depth, width), BF16),
            pltpu.VMEM((L, chunks, width, depth), BF16),
            pltpu.VMEM((2, Q, half, 2 * width), F32),
            pltpu.VMEM((2, Q - narrow, half, 2 * width), F32),
            pltpu.VMEM((2, narrow, half, 2 * width), BF16),
            pltpu.VMEM((2, Q, half, 2 * width), BF16),
            pltpu.VMEM((L, 2, Q, half, width), BF16),
            pltpu.VMEM((GROUPS, 2, half, depth), F32),
            pltpu.VMEM((GROUPS, 2, bits, half, depth), FOLD[0]),
            pltpu.VMEM((GROUPS, 2, bits, half, depth), FOLD[1]),
            pltpu.VMEM((GROUPS, 2, bits, half, depth), FOLD[0]),
            pltpu.VMEM((GROUPS, 2, bits, half, depth), FOLD[1]),
            pltpu.VMEM((L, GROUPS, R, 8, padded), F32),
            dma,
            dma((L, chunks)),
            dma((L, chunks)),
            dma((L, chunks)),
            dma((L, 2, Q)),
            dma((L, 2, Q)),
            dma((L, 2, Q)),
            dma((L, 2, Q)),
            dma((L, GROUPS, 2, bits)),
            dma((L, GROUPS, 2, bits)),
            dma((L, GROUPS, R)),
            dma((L, GROUPS, R)),
        ],
        compiler_params=pltpu.CompilerParams(
            collective_id=0, has_side_effects=True, vmem_limit_bytes=67043328
        ),
    )(tokens, g0, u0, d0, line(a0), line(b0), g1, u1, d1, line(a1), line(b1))


def solution(mesh):
    in_specs = (
        P("dp", "ra"),
        P("ra", "cb"),
        P("ra", "cb"),
        P("cb", "ra"),
        P("ra"),
        P("ra"),
        P("ra", "cb"),
        P("ra", "cb"),
        P("cb", "ra"),
        P("ra"),
        P("ra"),
    )

    def step(tokens, *rest):
        R, C = mesh.shape["ra"], mesh.shape["cb"]
        return on_device(R, C, tokens.shape[1] * R, tokens, *rest)

    return jax.shard_map(
        step, mesh=mesh, in_specs=in_specs, out_specs=P("dp", "ra"), check_vma=False
    )
```
